32 devices in a mesh: sp: 16 (over z, y, core), tp: 2 (over x).
Axes of the slice: x: 2, y: 2, z: 4, core: 2. Of those that a mesh axis runs over, the one named last changes fastest.
Arguments:
- tokens: bfloat16 [4096, 2048], P(('sp', 'tp')), may hold values from -96 to 96
- norm_gain: float32 [2048], replicated, may hold values from 0.1 to 1.9
- w_query: bfloat16 [2048, 1024], P(None, 'tp'), may hold values from -0.3 to 0.3
- w_key: bfloat16 [2048, 1024], P(None, 'tp'), may hold values from -0.3 to 0.3
- w_value: bfloat16 [2048, 1024], P(None, 'tp'), may hold values from -0.125 to 0.125
- w_att_gate: bfloat16 [2048, 1024], P(None, 'tp'), may hold values from -0.125 to 0.125
- w_rec_in: bfloat16 [2048, 1024], P(None, 'tp'), may hold values from -0.125 to 0.125
- w_rec_gate: bfloat16 [2048, 1024], P(None, 'tp'), may hold values from -0.125 to 0.125
- conv_taps: float32 [4, 1024], P(None, 'tp'), may hold values from -3 to 3
- gate_recur: bfloat16 [8, 128, 128], P('tp'), may hold values from -0.5 to 0.5
- gate_input: bfloat16 [8, 128, 128], P('tp'), may hold values from -0.5 to 0.5
- decay_rate: float32 [1024], P('tp'), may hold values from 1e-06 to 0.02
- head_lambda: float32 [8], P('tp'), may hold values from 0.3 to 0.8
- head_gain: float32 [1024], P('tp'), may hold values from 0.1 to 1.9
- out_att: bfloat16 [1024, 2048], P('tp'), may hold values from -0.125 to 0.125
- out_rec: bfloat16 [1024, 2048], P('tp'), may hold values from -0.125 to 0.125
Outputs:
- layer_out: bfloat16 [4096, 2048], P(('sp', 'tp'))
The draws below stay inside these ranges and needn't reach their ends.
All inputs are finite; a program needn't handle non-finite values.
Results may differ from the reference program's by a relative error of at most 0.015.
Values may be sent and summed in bfloat16 or wider, within the bound.
A program may use at most 128 MiB of HBM per device.

```python
import math
import jax
import jax.numpy as jnp
from jax import lax

D = 2048
HEADS = 8
HEAD_DIM = 64
V_DIM = 128
CHANNELS = 1024
GATE_BLOCK = 128
CONV = 4
TOKENS = 4096
BLOCKS = 8


WEIGHT_EDGE = 0.296875


def projection_base(key, salt):
    spread = 1.0 / math.sqrt(D * 4 // 7)
    base = jax.random.truncated_normal(jax.random.fold_in(key, salt), -6.0, 6.0, (D, HEADS * 2 * HEAD_DIM), jnp.float32)
    return jnp.clip(base * spread, -WEIGHT_EDGE, WEIGHT_EDGE)


def draw_w_query(key, part):
    weight = projection_base(key, 7003)
    return weight.astype(jnp.bfloat16)


def draw_w_key(key, part):
    weight = projection_base(key, 7004)
    return weight.astype(jnp.bfloat16)


def draw_tokens(key, part):
    values = jax.random.truncated_normal(jax.random.fold_in(key, 7005), -6.0, 6.0, (TOKENS, D), jnp.float32)
    return values.astype(jnp.bfloat16)


def shard_levels(stream_key, shape, pieces, low, largest):
    def one(dim, parts):
        steps = jax.random.uniform(jax.random.fold_in(jax.random.fold_in(stream_key, 6), dim), (parts,), jnp.float32, low / len(pieces), largest / len(pieces))
        return jnp.repeat(jnp.exp(steps), shape[dim] // parts).reshape((-1,) + (1,) * (len(shape) - dim - 1))

    level = one(*pieces[0])
    for cut in pieces[1:]:
        level = level * one(*cut)
    return level


def gaussian(rng, extent, deviation, reach, shards=(), kind=jnp.bfloat16):
    drawn = jax.random.normal(rng, extent, jnp.float32) * deviation
    if len(shards) > 0:
        drawn = shard_levels(rng, extent, shards, -0.22, 0.18) * drawn
    return jnp.clip(drawn, min=-reach, max=reach).astype(kind)


def setup_inputs(seed: int = 0) -> dict:
    key_list = jax.random.split(jax.random.key(seed), 17)
    tokens = draw_tokens(jax.random.fold_in(key_list[16], 71), 0)
    norm_gain = jnp.clip(1.0 + 0.18 * jax.random.normal(key_list[1], (D,), jnp.float32), 0.1, 1.9)
    w_query = draw_w_query(jax.random.fold_in(key_list[16], 71), 0)
    w_key = draw_w_key(jax.random.fold_in(key_list[16], 71), 0)
    w_value = gaussian(key_list[4], (D, HEADS * V_DIM), D ** -0.5, 0.125, ((1, 2),))
    w_att_gate = gaussian(key_list[5], (D, HEADS * V_DIM), D ** -0.5, 0.125, ((1, 2),))
    w_rec_in = gaussian(key_list[6], (D, CHANNELS), D ** -0.5, 0.125, ((1, 2),))
    w_rec_gate = gaussian(key_list[7], (D, CHANNELS), D ** -0.5, 0.125, ((1, 2),))
    conv_taps = gaussian(key_list[8], (CONV, CHANNELS), CONV ** -0.5, 3.0, ((1, 2),), jnp.float32)
    gate_recur = gaussian(key_list[9], (BLOCKS, GATE_BLOCK, GATE_BLOCK), GATE_BLOCK ** -0.5, 0.5, ((0, 2),))
    gate_input = gaussian(key_list[10], (BLOCKS, GATE_BLOCK, GATE_BLOCK), GATE_BLOCK ** -0.5, 0.5, ((0, 2),))
    decay_rate = jnp.clip(jnp.exp(math.log(0.02) - 9.9034875 * jax.random.uniform(key_list[11], (CHANNELS,), jnp.float32) ** shard_levels(key_list[11], (CHANNELS,), ((0, 2),), -0.2, 0.2)), 9.999999974752427e-07, 0.02)
    head_lambda = jnp.clip(0.3 + 0.5 * jax.random.uniform(key_list[12], (HEADS,), jnp.float32) ** shard_levels(key_list[12], (HEADS,), ((0, 2),), -0.2, 0.2), 0.3, 0.8)
    head_gain = jnp.clip(1.0 + 0.18 * jax.random.normal(key_list[13], (HEADS * V_DIM,), jnp.float32), 0.1, 1.9)
    out_att = gaussian(key_list[14], (HEADS * V_DIM, D), (HEADS * V_DIM + CHANNELS) ** -0.5, 0.125, ((0, 2),))
    out_rec = gaussian(key_list[15], (CHANNELS, D), (HEADS * V_DIM + CHANNELS) ** -0.5, 0.125, ((0, 2),))
    return {"tokens": tokens, "norm_gain": norm_gain, "w_query": w_query, "w_key": w_key, "w_value": w_value, "w_att_gate": w_att_gate, "w_rec_in": w_rec_in, "w_rec_gate": w_rec_gate, "conv_taps": conv_taps, "gate_recur": gate_recur, "gate_input": gate_input, "decay_rate": decay_rate, "head_lambda": head_lambda, "head_gain": head_gain, "out_att": out_att, "out_rec": out_rec}


EPS_INPUT = 1e-06
EPS_HEAD = 1e-05
RATE_SCALE = 8.0
HEAD_FACTOR = 0.8
MASKED = -1e+30

def rms_rows(values, gain, epsilon):
    mean_square = lax.optimization_barrier(jnp.mean(values * values, axis=-1, keepdims=True))
    return values * lax.rsqrt(mean_square + epsilon) * gain

def combine_pair(earlier, later):
    return (earlier[0] * later[0], later[0] * earlier[1] + later[1])

def reference(tokens, norm_gain, w_query, w_key, w_value, w_att_gate, w_rec_in, w_rec_gate, conv_taps, gate_recur, gate_input, decay_rate, head_lambda, head_gain, out_att, out_rec):
    normed = rms_rows(tokens.astype(jnp.float32), norm_gain, EPS_INPUT).astype(jnp.bfloat16)

    def project(weight):
        return jnp.dot(normed, weight, preferred_element_type=jnp.float32).astype(jnp.bfloat16)
    queries = project(w_query).reshape(TOKENS, HEADS, 2, HEAD_DIM)
    keys = project(w_key).reshape(TOKENS, HEADS, 2, HEAD_DIM)
    values = project(w_value).reshape(TOKENS, HEADS, V_DIM)
    att_gate = project(w_att_gate)
    rec_in = project(w_rec_in)
    rec_gate = project(w_rec_gate)
    block_rows = math.gcd(TOKENS, 512)
    scale = HEAD_DIM ** (-0.5)
    key_pos = jnp.arange(TOKENS, dtype=jnp.int32)

    def one_head(operands):
        head_query, head_key, head_value, weight_lambda = operands

        def one_block(index):
            anchor = (index * block_rows).astype(jnp.int32)
            query_block = lax.dynamic_slice_in_dim(head_query, anchor, block_rows, 0)
            query_pos = anchor + jnp.arange(block_rows, dtype=jnp.int32)
            allowed = key_pos[None, :] <= query_pos[:, None]

            def weighted_of(which):
                scores = jnp.dot(query_block[:, which], head_key[:, which].T, preferred_element_type=jnp.float32) * scale
                scores = jnp.where(allowed, scores, MASKED)
                top = lax.optimization_barrier(jnp.max(scores, axis=-1, keepdims=True))
                raised = jnp.where(allowed, jnp.exp(scores - top), 0.0)
                total = lax.optimization_barrier(jnp.sum(raised, axis=-1, keepdims=True))
                weighted = jnp.dot(raised.astype(jnp.bfloat16), head_value, preferred_element_type=jnp.float32)
                return weighted / total
            return weighted_of(0) - weight_lambda * weighted_of(1)
        blocks = lax.map(one_block, jnp.arange(TOKENS // block_rows, dtype=jnp.int32))
        return blocks.reshape(TOKENS, V_DIM)
    per_head = lax.map(one_head, (jnp.moveaxis(queries, 1, 0), jnp.moveaxis(keys, 1, 0), jnp.moveaxis(values, 1, 0), head_lambda))
    head_out = rms_rows(per_head, head_gain.reshape(HEADS, 1, V_DIM), EPS_HEAD) * HEAD_FACTOR
    head_out = jnp.moveaxis(head_out, 0, 1).reshape(TOKENS, HEADS * V_DIM)
    att_mixed = (head_out * jax.nn.silu(att_gate.astype(jnp.float32))).astype(jnp.bfloat16)
    padded = jnp.concatenate([jnp.zeros((CONV - 1, CHANNELS), jnp.bfloat16), rec_in], axis=0).astype(jnp.float32)
    conv_sum = jnp.zeros((TOKENS, CHANNELS), jnp.float32)
    for offset in range(CONV):
        conv_sum = conv_sum + padded[offset:offset + TOKENS] * conv_taps[offset]
    conv_out = conv_sum.astype(jnp.bfloat16)
    grouped = conv_out.reshape(TOKENS, BLOCKS, GATE_BLOCK).astype(jnp.float32)
    recur_gate = jax.nn.sigmoid(jnp.einsum('tnc,ncd->tnd', grouped, gate_recur.astype(jnp.float32)).reshape(TOKENS, CHANNELS))
    inflow = jax.nn.sigmoid(jnp.einsum('tnc,ncd->tnd', grouped, gate_input.astype(jnp.float32)).reshape(TOKENS, CHANNELS))
    log_decay = -RATE_SCALE * recur_gate * decay_rate
    decays = jnp.exp(log_decay)
    at_anchor = (jnp.arange(TOKENS, dtype=jnp.int32) == 0)[:, None]
    norm_in = jnp.where(at_anchor, 1.0, jnp.sqrt(-jnp.expm1(2.0 * log_decay)))
    driven = norm_in * inflow * conv_out.astype(jnp.float32)
    _, states = lax.associative_scan(combine_pair, (decays, driven), axis=0)
    rec_mixed = (states * jax.nn.silu(rec_gate.astype(jnp.float32))).astype(jnp.bfloat16)
    output = jnp.dot(att_mixed, out_att, preferred_element_type=jnp.float32) + jnp.dot(rec_mixed, out_rec, preferred_element_type=jnp.float32)
    return output.astype(jnp.bfloat16)
```

```python
import functools

import jax
import jax.numpy as jnp
from jax import lax
from jax.experimental import pallas as pl
from jax.experimental.pallas import tpu as pltpu
from jax.sharding import PartitionSpec as P

EPS_INPUT = 1e-06
EPS_HEAD = 1e-05
RATE_SCALE = 8.0
HEAD_FACTOR = 0.8
MASKED = -1e30


def passed_along(block, axis, distance):
    devices = range(lax.axis_size(axis))
    route = [(i - distance, i) for i in devices if i - distance in devices]
    return lax.ppermute(block, axis, route)


def rms_rows(values, gain, epsilon):
    mean_square = jnp.mean(values * values, axis=-1, keepdims=True)
    return values * lax.rsqrt(mean_square + epsilon) * gain


def attn_kernel(plane, idx_ref, lam_ref, q_ref, kv_ref, gain_ref, o_ref, m_ref, l_ref, acc_ref):
    rows = q_ref.shape[1]
    width = q_ref.shape[2]
    half = width // 2
    mine = pl.program_id(0) * plane + idx_ref[0]
    q = q_ref[0].astype(jnp.float32) * (half ** (-0.5))
    lane = lax.broadcasted_iota(jnp.int32, q.shape, 1)
    both = jnp.concatenate(
        [jnp.where(lane < half, q, 0.0), jnp.where(lane >= half, q, 0.0)], axis=0
    ).astype(jnp.bfloat16)
    m_ref[...] = jnp.full(m_ref.shape, MASKED, jnp.float32)
    l_ref[...] = jnp.zeros(l_ref.shape, jnp.float32)
    acc_ref[...] = jnp.zeros(acc_ref.shape, jnp.float32)

    def step(pair, masked):
        first = 2 * pair
        r, z = lax.rem(first, plane), lax.div(first, plane)
        keys = jnp.concatenate([kv_ref[r, z, :, :width], kv_ref[r + 1, z, :, :width]], axis=0)
        vals = jnp.concatenate([kv_ref[r, z, :, width:], kv_ref[r + 1, z, :, width:]], axis=0)
        s = lax.dot_general(
            both, keys, (((1,), (1,)), ((), ())), preferred_element_type=jnp.float32
        )
        if masked:
            qpos = lax.rem(lax.broadcasted_iota(jnp.int32, s.shape, 0), rows) + mine * rows
            kpos = lax.broadcasted_iota(jnp.int32, s.shape, 1) + first * rows
            s = jnp.where(kpos <= qpos, s, MASKED)
        old = m_ref[...]
        new = jnp.maximum(old, jnp.max(s, axis=-1, keepdims=True))
        factor = jnp.exp(old - new)
        p = jnp.exp(s - new[:, :1])
        m_ref[...] = new
        part = p[:, :128]
        for c in range(1, s.shape[1] // 128):
            part = part + p[:, c * 128 : (c + 1) * 128]
        l_ref[...] = l_ref[...] * factor + part
        acc_ref[...] = acc_ref[...] * factor + jnp.dot(
            p.astype(jnp.bfloat16), vals, preferred_element_type=jnp.float32
        )

    def body(pair, _):
        step(pair, False)
        return 0

    last = lax.div(mine, 2)
    lax.fori_loop(0, last, body, 0)
    step(last, True)
    total = jnp.sum(l_ref[...], axis=-1, keepdims=True)
    out = acc_ref[...] / total
    per_head = out[:rows] - lam_ref[0] * out[rows:]
    o_ref[0] = (rms_rows(per_head, gain_ref[...], EPS_HEAD) * HEAD_FACTOR).astype(o_ref.dtype)


def attention(queries, keys, values, head_lambda, head_gain):
    rows = queries.shape[0]
    heads = head_lambda.shape[0]
    sp = lax.axis_size("sp")
    plane = sp // heads
    strided = [[r + plane * g for g in range(heads)] for r in range(plane)]
    planes = [[r + plane * g for r in range(plane)] for g in range(heads)]
    width = queries.shape[1] // heads
    vdim = values.shape[1] // heads
    packed = jnp.concatenate(
        [part.reshape(rows, heads, -1).swapaxes(0, 1) for part in (queries, keys, values)], axis=2
    )
    mixed = lax.all_to_all(
        packed, "sp", split_axis=0, concat_axis=0, tiled=True, axis_index_groups=strided
    )
    kv = lax.all_gather(mixed[:, :, width:], "sp", axis=0, axis_index_groups=planes)
    index = lax.axis_index("sp")
    head = index // plane
    lam = lax.dynamic_slice_in_dim(head_lambda, head, 1)
    gain = lax.dynamic_slice_in_dim(head_gain.reshape(heads, vdim), head, 1, 0)
    out = pl.pallas_call(
        functools.partial(attn_kernel, plane),
        grid=(heads,),
        out_shape=jax.ShapeDtypeStruct((heads, rows, vdim), jnp.bfloat16),
        in_specs=[
            pl.BlockSpec(memory_space=pltpu.SMEM),
            pl.BlockSpec(memory_space=pltpu.SMEM),
            pl.BlockSpec((1, rows, width), lambda g: (g, 0, 0)),
            pl.BlockSpec(memory_space=pltpu.VMEM),
            pl.BlockSpec(memory_space=pltpu.VMEM),
        ],
        out_specs=pl.BlockSpec((1, rows, vdim), lambda g: (g, 0, 0)),
        scratch_shapes=[
            pltpu.VMEM((2 * rows, 128), jnp.float32),
            pltpu.VMEM((2 * rows, 128), jnp.float32),
            pltpu.VMEM((2 * rows, vdim), jnp.float32),
        ],
        name="attn",
    )((index % plane).astype(jnp.int32).reshape(1), lam, mixed[:, :, :width], kv, gain)
    back = lax.all_to_all(
        out, "sp", split_axis=0, concat_axis=0, tiled=True, axis_index_groups=strided
    )
    return back.swapaxes(0, 1).reshape(rows, heads * vdim)


def scan_kernel(idx_ref, rec_ref, early_ref, taps_ref, gr_ref, gi_ref, rate_ref, p_ref, s_ref):
    rows, width = rec_ref.shape
    taps = taps_ref.shape[0]
    at = lax.broadcasted_iota(jnp.int32, (rows, width), 0)
    x = rec_ref[...].astype(jnp.float32)
    early = early_ref[...].astype(jnp.float32)
    conv = jnp.zeros((rows, width), jnp.float32)
    for offset in range(taps):
        back = taps - 1 - offset
        if back:
            moved = pltpu.roll(x, back, 0)
            for row in range(back):
                moved = jnp.where(at == row, early[taps - 1 - back + row][None], moved)
        else:
            moved = x
        conv = conv + moved * taps_ref[offset][None]
    conv16 = conv.astype(jnp.bfloat16)
    size = gr_ref.shape[1]
    gates, flows = [], []
    for n in range(gr_ref.shape[0]):
        piece = conv16[:, n * size : (n + 1) * size]
        gates.append(jnp.dot(piece, gr_ref[n], preferred_element_type=jnp.float32))
        flows.append(jnp.dot(piece, gi_ref[n], preferred_element_type=jnp.float32))
    recur = jax.nn.sigmoid(jnp.concatenate(gates, axis=1))
    inflow = jax.nn.sigmoid(jnp.concatenate(flows, axis=1))
    log_decay = -RATE_SCALE * recur * rate_ref[...]
    a = jnp.exp(log_decay)
    y = 2.0 * log_decay
    small = -y * (1.0 + y * (1 / 2) * (1.0 + y * (1 / 3) * (1.0 + y * (1 / 4) * (1.0 + y * (1 / 5) * (1.0 + y * (1 / 6))))))
    fall = jnp.where(y > -0.35, small, 1.0 - jnp.exp(y))
    norm_in = jnp.where((at == 0) & (idx_ref[0] == 0), 1.0, jnp.sqrt(fall))
    b = norm_in * inflow * conv16.astype(jnp.float32)
    shift = 1
    while shift < rows:
        keep = at >= shift
        pa = jnp.where(keep, pltpu.roll(a, shift, 0), 1.0)
        pb = jnp.where(keep, pltpu.roll(b, shift, 0), 0.0)
        b = b + a * pb
        a = a * pa
        shift *= 2
    p_ref[...] = a
    s_ref[...] = b


def recurrence(rec_in, rec_gate, conv_taps, gate_recur, gate_input, decay_rate):
    rows, width = rec_in.shape
    taps = conv_taps.shape[0]
    early = passed_along(rec_in[rows - (taps - 1) :], "sp", 1)
    mine = lax.axis_index("sp")
    products, partial_states = pl.pallas_call(
        scan_kernel,
        out_shape=[jax.ShapeDtypeStruct((rows, width), jnp.float32)] * 2,
        in_specs=[pl.BlockSpec(memory_space=pltpu.SMEM)]
        + [pl.BlockSpec(memory_space=pltpu.VMEM)] * 6,
        out_specs=[pl.BlockSpec(memory_space=pltpu.VMEM)] * 2,
        name="scan",
    )(
        mine.astype(jnp.int32).reshape(1),
        rec_in,
        early,
        conv_taps,
        gate_recur,
        gate_input,
        decay_rate.reshape(1, width),
    )
    ends = jnp.concatenate([products[rows - 1 :], partial_states[rows - 1 :]], axis=0)
    pieces = lax.all_gather(ends, "sp")
    carry = jnp.zeros((width,), jnp.float32)
    for position in range(lax.axis_size("sp") - 1):
        longer = pieces[position, 0] * carry + pieces[position, 1]
        carry = jnp.where(position < mine, longer, carry)
    states = partial_states + products * carry[None, :]
    return (states * jax.nn.silu(rec_gate.astype(jnp.float32))).astype(jnp.bfloat16)


def body(
    tokens,
    norm_gain,
    w_query,
    w_key,
    w_value,
    w_att_gate,
    w_rec_in,
    w_rec_gate,
    conv_taps,
    gate_recur,
    gate_input,
    decay_rate,
    head_lambda,
    head_gain,
    out_att,
    out_rec,
):
    tp = lax.axis_size("tp")
    normed = rms_rows(tokens.astype(jnp.float32), norm_gain, EPS_INPUT).astype(jnp.bfloat16)
    whole = lax.all_gather(normed, "tp", axis=0, tiled=True)
    queries, keys, values, att_gate, rec_in, rec_gate = [
        jnp.dot(whole, weight, preferred_element_type=jnp.float32).astype(jnp.bfloat16)
        for weight in (w_query, w_key, w_value, w_att_gate, w_rec_in, w_rec_gate)
    ]
    head_out = attention(queries, keys, values, head_lambda, head_gain)
    att_mixed = (
        head_out.astype(jnp.float32) * jax.nn.silu(att_gate.astype(jnp.float32))
    ).astype(jnp.bfloat16)
    rec_mixed = recurrence(rec_in, rec_gate, conv_taps, gate_recur, gate_input, decay_rate)
    partial = jnp.dot(att_mixed, out_att, preferred_element_type=jnp.float32) + jnp.dot(
        rec_mixed, out_rec, preferred_element_type=jnp.float32
    )
    partial = partial.astype(jnp.bfloat16).reshape(tp, -1, partial.shape[1])
    parts = lax.all_to_all(partial, "tp", split_axis=0, concat_axis=0, tiled=True)
    return jnp.sum(parts.astype(jnp.float32), axis=0).astype(jnp.bfloat16)


def solution(mesh):
    return jax.shard_map(
        body,
        mesh=mesh,
        in_specs=(
            P(("sp", "tp"), None),
            P(),
            P(None, "tp"),
            P(None, "tp"),
            P(None, "tp"),
            P(None, "tp"),
            P(None, "tp"),
            P(None, "tp"),
            P(None, "tp"),
            P("tp", None, None),
            P("tp", None, None),
            P("tp"),
            P("tp"),
            P("tp"),
            P("tp", None),
            P("tp", None),
        ),
        out_specs=P(("sp", "tp"), None),
        check_vma=False,
    )
```

```python
import functools

import jax
import jax.numpy as jnp
from jax import lax
from jax.experimental import pallas as pl
from jax.experimental.pallas import tpu as pltpu
from jax.sharding import PartitionSpec as P

EPS_INPUT = 1e-06
EPS_HEAD = 1e-05
RATE_SCALE = 8.0
HEAD_FACTOR = 0.8
MASKED = -1e30
MESH = pl.DeviceIdType.MESH
VMEM = pl.BlockSpec(memory_space=pltpu.VMEM)
ANY = pl.BlockSpec(memory_space=pl.ANY)
SMEM = pl.BlockSpec(memory_space=pltpu.SMEM)
LIMIT = 60 * 1024 * 1024


def rms_rows(values, gain, epsilon):
    mean_square = jnp.mean(values * values, axis=-1, keepdims=True)
    return values * lax.rsqrt(mean_square + epsilon) * gain


def greet(axis, size):
    barrier = pltpu.get_barrier_semaphore()
    me = lax.axis_index(axis)

    def one(k, _):
        pl.semaphore_signal(
            barrier, inc=1, device_id={axis: lax.rem(me + k, size)}, device_id_type=MESH
        )
        return 0

    lax.fori_loop(1, size, one, 0)


def remote(src, dst, send, recv, device):
    return pltpu.make_async_remote_copy(
        src_ref=src, dst_ref=dst, send_sem=send, recv_sem=recv, device_id=device, device_id_type=MESH
    )


def fall_of(y):
    series = 1.0 + y * (1 / 6)
    for n in (5, 4, 3, 2):
        series = 1.0 + y * (1 / n) * series
    return jnp.where(y > -0.35, -y * series, 1.0 - jnp.exp(y))


def front_kernel(
    tp,
    sp,
    heads,
    tok_ref,
    ngain_ref,
    wq,
    wk,
    wv,
    wri,
    wag,
    wrg,
    taps_ref,
    gr_ref,
    gi_ref,
    rate_ref,
    q_out,
    kv_out,
    ag_out,
    rg_out,
    prod_out,
    state_out,
    ends_out,
    w_buf,
    x_all,
    q_pack,
    kv_pack,
    ri_buf,
    tail_buf,
    early_buf,
    my_end,
    wsem,
    xs,
    xr,
    qs,
    qr,
    ks,
    kr,
    as_,
    ar,
    bs,
    br,
    hs,
    hr,
    es,
    er,
):
    me, col = lax.axis_index("sp"), lax.axis_index("tp")
    plane = sp // heads
    lanes = plane // 2
    z, r = lax.div(me, plane), lax.rem(me, plane)
    part_rows = tok_ref.shape[0]
    rows, width = prod_out.shape
    qw = q_out.shape[3]
    kvw = kv_out.shape[4]
    weights = [pltpu.make_async_copy(w, w_buf.at[n], wsem.at[n]) for n, w in enumerate((wq, wk, wv, wri, wag, wrg))]
    for copy in weights:
        copy.start()
    greet("sp", sp)
    greet("tp", tp)
    x_all[col] = rms_rows(tok_ref[...].astype(jnp.float32), ngain_ref[...], EPS_INPUT).astype(jnp.bfloat16)
    pl.semaphore_wait(pltpu.get_barrier_semaphore(), sp + tp - 2)

    def give(k):
        return remote(x_all.at[col], x_all.at[col], xs.at[k], xr.at[k], {"tp": lax.rem(col + k, tp)})

    for k in range(1, tp):
        give(k).start()

    def dot(t, n):
        return jnp.dot(x_all[t], w_buf[n], preferred_element_type=jnp.float32).astype(jnp.bfloat16)

    def spread(k, s, t):
        there = {"sp": lax.rem(z + k, heads) * plane + r}
        n = k * tp + s
        g = lax.rem(z + k, heads)
        return (
            remote(kv_pack.at[g, s], kv_out.at[r, z, t], ks.at[n], kr.at[n], there),
            remote(q_pack.at[g, s], q_out.at[z, t], qs.at[n], qr.at[n], there),
        )

    def across(m, k, s, t):
        src = kv_out.at[r, lax.rem(z - k + heads, heads), t]
        n = (m * heads + k) * tp + s
        return remote(src, src, as_.at[n], ar.at[n], {"sp": z * plane + lax.rem(r + 2 * m, plane)})

    def twin(m, k, s, t):
        src = kv_out.at[lax.rem(r - 2 * m + plane, plane), lax.rem(z - k + heads, heads), t]
        n = (m * heads + k) * tp + s
        return remote(src, src, bs.at[n], br.at[n], {"sp": z * plane + r + 1 - 2 * lax.rem(r, 2)})

    def loop(low, high, fn):
        def one(m, _):
            fn(m)
            return 0

        lax.fori_loop(low, high, one, 0)

    def service(s, t):
        for k in range(heads):
            if k:
                spread(k, s, t)[0].wait_recv()
            loop(1, lanes, lambda m: across(m, k, s, t).start())
            twin(0, k, s, t).start()

    turns = [lax.rem(col - s + tp, tp) for s in range(tp)]
    for s, t in enumerate(turns):
        if s:
            give(s).wait_recv()
        at = pl.ds(pl.multiple_of(t * part_rows, part_rows), part_rows)
        for n in range(3):
            if s == 0:
                weights[n].wait()
            piece = dot(t, n)
            for g in range(heads):
                block = piece[:, g * qw : (g + 1) * qw]
                if n == 0:
                    q_pack[g, s] = block
                else:
                    kv_pack[g, s, :, (n - 1) * qw : n * qw] = block
        kv_out[r, z, t] = kv_pack[z, s]
        q_out[z, t] = q_pack[z, s]
        for k in range(1, heads):
            for copy in spread(k, s, t):
                copy.start()
        if s == 0:
            weights[3].wait()
        ri_buf[at] = dot(t, 3)
        if s:
            service(s - 1, turns[s - 1])
    tail_buf[...] = ri_buf[rows - 16 :]
    halo = remote(tail_buf, early_buf, hs, hr, {"sp": lax.rem(me + 1, sp)})
    halo.start()
    weights[4].wait()
    weights[5].wait()
    for t in range(tp):
        ag_out[t * part_rows : (t + 1) * part_rows] = dot(t, 4)
        rg_out[t * part_rows : (t + 1) * part_rows] = dot(t, 5)
    halo.wait()

    at = lax.broadcasted_iota(jnp.int32, (rows, width), 0)
    taps = taps_ref.shape[0]
    x = ri_buf[...].astype(jnp.float32)
    early = jnp.where(me == 0, 0.0, early_buf[...].astype(jnp.float32))
    conv = x * taps_ref[taps - 1][None]
    for back in range(1, taps):
        moved = pltpu.roll(x, back, 0)
        for row in range(back):
            moved = jnp.where(at == row, early[16 - back + row][None], moved)
        conv = conv + moved * taps_ref[taps - 1 - back][None]
    conv16 = conv.astype(jnp.bfloat16)
    size = gr_ref.shape[1]
    gates, flows = [], []
    for n in range(gr_ref.shape[0]):
        piece = conv16[:, n * size : (n + 1) * size]
        gates.append(jnp.dot(piece, gr_ref[n], preferred_element_type=jnp.float32))
        flows.append(jnp.dot(piece, gi_ref[n], preferred_element_type=jnp.float32))
    recur = jax.nn.sigmoid(jnp.concatenate(gates, axis=1))
    inflow = jax.nn.sigmoid(jnp.concatenate(flows, axis=1))
    log_decay = -RATE_SCALE * recur * rate_ref[...]
    a = jnp.exp(log_decay)
    norm_in = jnp.where((at == 0) & (me == 0), 1.0, jnp.sqrt(fall_of(2.0 * log_decay)))
    b = norm_in * inflow * conv16.astype(jnp.float32)
    shift = 1
    while shift < rows:
        keep = at >= shift
        pa = jnp.where(keep, pltpu.roll(a, shift, 0), 1.0)
        pb = jnp.where(keep, pltpu.roll(b, shift, 0), 0.0)
        b = b + a * pb
        a = a * pa
        shift *= 2
    prod_out[...] = a
    state_out[...] = b
    my_end[...] = jnp.zeros(my_end.shape, jnp.float32)
    my_end[0:1] = a[rows - 1 :]
    my_end[1:2] = b[rows - 1 :]
    ends_out[me] = my_end[...]

    def end(k):
        return remote(my_end, ends_out.at[me], es.at[k], er.at[k], {"sp": lax.rem(me + k, sp)})

    loop(1, sp, lambda k: end(k).start())
    service(tp - 1, turns[tp - 1])
    for s, t in enumerate(turns):
        for k in range(heads):

            def on(m):
                across(m, k, s, t).wait_recv()
                twin(m, k, s, t).start()

            loop(1, lanes, on)
    for s, t in enumerate(turns):
        for k in range(heads):
            if k:
                kv_copy, q_copy = spread(k, s, t)
                kv_copy.wait_send()
                q_copy.wait()
            loop(1, lanes, lambda m: across(m, k, s, t).wait_send())
            loop(0, lanes, lambda m: twin(m, k, s, t).wait())
    for k in range(1, tp):
        give(k).wait_send()
    loop(1, sp, lambda k: end(k).wait())


def back_kernel(
    tp,
    sp,
    heads,
    lam_ref,
    q_ref,
    kv_ref,
    ag_ref,
    rg_ref,
    prod_ref,
    state_ref,
    ends_ref,
    gain_ref,
    oa_hbm,
    or_hbm,
    out_ref,
    oa,
    orr,
    m_ref,
    l_ref,
    acc_ref,
    o_stage,
    o_all,
    rec_part,
    p_stage,
    p_all,
    wsem,
    osd,
    ord_,
    ps,
    pr,
):
    me, col = lax.axis_index("sp"), lax.axis_index("tp")
    plane = sp // heads
    z, r = lax.div(me, plane), lax.rem(me, plane)
    part_rows = q_ref.shape[2]
    rows = tp * part_rows
    width = q_ref.shape[3]
    half = width // 2
    w1 = pltpu.make_async_copy(oa_hbm, oa, wsem.at[0])
    w2 = pltpu.make_async_copy(or_hbm, orr, wsem.at[1])
    w1.start()
    w2.start()
    barrier = pltpu.get_barrier_semaphore()
    for k in range(1, heads):
        pl.semaphore_signal(
            barrier, inc=1, device_id={"sp": lax.rem(z + k, heads) * plane + r}, device_id_type=MESH
        )
    greet("tp", tp)
    pl.semaphore_wait(barrier, heads + tp - 2)
    lane = lax.broadcasted_iota(jnp.int32, (rows, width), 1)

    def give(k):
        g = lax.rem(z + k, heads)
        return remote(o_stage.at[g], o_all.at[z], osd.at[k], ord_.at[k], {"sp": g * plane + r})

    def attend(g):
        mine = g * plane + r
        q = q_ref[g].reshape(rows, width).astype(jnp.float32) * (half ** (-0.5))
        both = (
            jnp.where(lane < half, q, 0.0).astype(jnp.bfloat16),
            jnp.where(lane >= half, q, 0.0).astype(jnp.bfloat16),
        )
        m_ref[...] = jnp.full(m_ref.shape, MASKED, jnp.float32)
        l_ref[...] = jnp.zeros(l_ref.shape, jnp.float32)
        acc_ref[...] = jnp.zeros(acc_ref.shape, jnp.float32)

        def step(pair, masked):
            first = 2 * pair
            at, zz = lax.rem(first, plane), lax.div(first, plane)
            block = kv_ref[pl.ds(at, 2), zz].reshape(2 * rows, -1)
            keys, vals = block[:, :width], block[:, width:]
            scores = [
                lax.dot_general(
                    q_p, keys, (((1,), (1,)), ((), ())), preferred_element_type=jnp.float32
                )
                for q_p in both
            ]
            for p, s in enumerate(scores):
                if masked:
                    qpos = lax.broadcasted_iota(jnp.int32, s.shape, 0) + mine * rows
                    kpos = lax.broadcasted_iota(jnp.int32, s.shape, 1) + first * rows
                    s = jnp.where(kpos <= qpos, s, MASKED)
                old = m_ref[p]
                new = jnp.maximum(old, jnp.max(s, axis=-1, keepdims=True))
                factor = jnp.exp(old - new)
                e = jnp.exp(s - new[:, :1])
                m_ref[p] = new
                part = e[:, :128]
                for c in range(1, s.shape[1] // 128):
                    part = part + e[:, c * 128 : (c + 1) * 128]
                l_ref[p] = l_ref[p] * factor + part
                acc_ref[p] = acc_ref[p] * factor + jnp.dot(
                    e.astype(jnp.bfloat16), vals, preferred_element_type=jnp.float32
                )

        def body(pair, _):
            step(pair, False)
            return 0

        last = lax.div(mine, 2)
        lax.fori_loop(0, last, body, 0)
        step(last, True)
        maps = [acc_ref[p] / jnp.sum(l_ref[p], axis=-1, keepdims=True) for p in range(2)]
        per_head = maps[0] - lam_ref[z] * maps[1]
        normal = rms_rows(per_head, gain_ref[pl.ds(z, 1)], EPS_HEAD) * HEAD_FACTOR
        return normal.astype(jnp.bfloat16)

    for k in list(range(1, heads)) + [0]:
        g = lax.rem(z + k, heads)
        done = attend(g)
        if k:
            o_stage[g] = done
            give(k).start()
        else:
            o_all[z] = done

    def hop(position, carry):
        longer = ends_ref[position, 0:1] * carry + ends_ref[position, 1:2]
        return jnp.where(position < me, longer, carry)

    carry = lax.fori_loop(0, sp - 1, hop, jnp.zeros((1, prod_ref.shape[1]), jnp.float32))
    states = state_ref[...] + prod_ref[...] * carry
    rec = (states * jax.nn.silu(rg_ref[...].astype(jnp.float32))).astype(jnp.bfloat16)
    w1.wait()
    w2.wait()
    rec_part[...] = jnp.dot(rec, orr[...], preferred_element_type=jnp.float32)
    for k in range(1, heads):
        give(k).wait()

    def partial(t):
        at = pl.ds(pl.multiple_of(t * part_rows, part_rows), part_rows)
        att = jnp.concatenate([o_all[h, at] for h in range(heads)], axis=1).astype(jnp.float32)
        mixed = (att * jax.nn.silu(ag_ref[at].astype(jnp.float32))).astype(jnp.bfloat16)
        return rec_part[at] + jnp.dot(mixed, oa[...], preferred_element_type=jnp.float32)

    def pass_on(k):
        t = lax.rem(col + k, tp)
        return remote(p_stage.at[t], p_all.at[col], ps.at[k], pr.at[k], {"tp": t})

    for k in range(1, tp):
        t = lax.rem(col + k, tp)
        p_stage[t] = partial(t).astype(jnp.bfloat16)
        pass_on(k).start()
    total = partial(col)
    for k in range(1, tp):
        pass_on(k).wait()
        total = total + p_all[lax.rem(col - k + tp, tp)].astype(jnp.float32)
    out_ref[...] = total.astype(jnp.bfloat16)


def body(
    tokens,
    norm_gain,
    w_query,
    w_key,
    w_value,
    w_att_gate,
    w_rec_in,
    w_rec_gate,
    conv_taps,
    gate_recur,
    gate_input,
    decay_rate,
    head_lambda,
    head_gain,
    out_att,
    out_rec,
):
    tp, sp, heads = lax.axis_size("tp"), lax.axis_size("sp"), head_lambda.shape[0]
    plane = sp // heads
    lanes = plane // 2
    part, depth = tokens.shape
    rows, width = part * tp, w_query.shape[1]
    qw, vdim = width // heads, w_value.shape[1] // heads
    kvw = qw + vdim
    chans = w_rec_in.shape[1]
    f32, b16 = jnp.float32, jnp.bfloat16
    shape = jax.ShapeDtypeStruct
    dma = pltpu.SemaphoreType.DMA
    steps = heads * tp
    q, kv, ag, rg, prod, state, ends = pl.pallas_call(
        functools.partial(front_kernel, tp, sp, heads),
        out_shape=[
            shape((heads, tp, part, qw), b16),
            shape((plane, heads, tp, part, kvw), b16),
            shape((rows, width), b16),
            shape((rows, chans), b16),
            shape((rows, chans), f32),
            shape((rows, chans), f32),
            shape((sp, 8, chans), f32),
        ],
        in_specs=[VMEM] * 2 + [ANY] * 6 + [VMEM] * 4,
        out_specs=[VMEM] * 7,
        scratch_shapes=[
            pltpu.VMEM((6, depth, width), b16),
            pltpu.VMEM((tp, part, depth), b16),
            pltpu.VMEM((heads, tp, part, qw), b16),
            pltpu.VMEM((heads, tp, part, kvw), b16),
            pltpu.VMEM((rows, chans), b16),
            pltpu.VMEM((16, chans), b16),
            pltpu.VMEM((16, chans), b16),
            pltpu.VMEM((8, chans), f32),
            dma((6,)),
            dma((tp,)),
            dma((tp,)),
            dma((steps,)),
            dma((steps,)),
            dma((steps,)),
            dma((steps,)),
            dma((lanes * steps,)),
            dma((lanes * steps,)),
            dma((lanes * steps,)),
            dma((lanes * steps,)),
            dma,
            dma,
            dma((sp,)),
            dma((sp,)),
        ],
        compiler_params=pltpu.CompilerParams(
            collective_id=0, has_side_effects=True, vmem_limit_bytes=LIMIT
        ),
        name="front",
    )(
        tokens,
        norm_gain.reshape(1, depth),
        w_query,
        w_key,
        w_value,
        w_rec_in,
        w_att_gate,
        w_rec_gate,
        conv_taps,
        gate_recur,
        gate_input,
        decay_rate.reshape(1, chans),
    )
    return pl.pallas_call(
        functools.partial(back_kernel, tp, sp, heads),
        out_shape=shape((part, out_att.shape[1]), b16),
        in_specs=[SMEM] + [VMEM] * 8 + [ANY] * 2,
        out_specs=VMEM,
        scratch_shapes=[
            pltpu.VMEM(out_att.shape, b16),
            pltpu.VMEM(out_rec.shape, b16),
            pltpu.VMEM((2, rows, 128), f32),
            pltpu.VMEM((2, rows, 128), f32),
            pltpu.VMEM((2, rows, vdim), f32),
            pltpu.VMEM((heads, rows, vdim), b16),
            pltpu.VMEM((heads, rows, vdim), b16),
            pltpu.VMEM((rows, out_att.shape[1]), f32),
            pltpu.VMEM((tp, part, out_att.shape[1]), b16),
            pltpu.VMEM((tp, part, out_att.shape[1]), b16),
            dma((2,)),
            dma((heads,)),
            dma((heads,)),
            dma((tp,)),
            dma((tp,)),
        ],
        compiler_params=pltpu.CompilerParams(
            collective_id=1, has_side_effects=True, vmem_limit_bytes=LIMIT
        ),
        name="back",
    )(head_lambda, q, kv, ag, rg, prod, state, ends, head_gain.reshape(heads, vdim), out_att, out_rec)


def solution(mesh):
    return jax.shard_map(
        body,
        mesh=mesh,
        in_specs=(
            P(("sp", "tp"), None),
            P(),
            P(None, "tp"),
            P(None, "tp"),
            P(None, "tp"),
            P(None, "tp"),
            P(None, "tp"),
            P(None, "tp"),
            P(None, "tp"),
            P("tp", None, None),
            P("tp", None, None),
            P("tp"),
            P("tp"),
            P("tp"),
            P("tp", None),
            P("tp", None),
        ),
        out_specs=P(("sp", "tp"), None),
        check_vma=False,
    )
```

```python
import functools
import math

import jax
import jax.numpy as jnp
from jax import lax
from jax.experimental import pallas as pl
from jax.experimental.pallas import tpu as pltpu
from jax.sharding import PartitionSpec as P

EPS_INPUT = 1e-06
EPS_HEAD = 1e-05
RATE_SCALE = 8.0
HEAD_FACTOR = 0.8
MASKED = -1e30
MESH = pl.DeviceIdType.MESH
VMEM = pl.BlockSpec(memory_space=pltpu.VMEM)
ANY = pl.BlockSpec(memory_space=pl.ANY)
SMEM = pl.BlockSpec(memory_space=pltpu.SMEM)
LIMIT = 60 * 1024 * 1024


def rms_rows(values, gain, epsilon):
    mean_square = jnp.mean(values * values, axis=-1, keepdims=True)
    return values * lax.rsqrt(mean_square + epsilon) * gain


def greet(axis, size):
    barrier = pltpu.get_barrier_semaphore()
    me = lax.axis_index(axis)

    def one(k, _):
        pl.semaphore_signal(
            barrier, inc=1, device_id={axis: lax.rem(me + k, size)}, device_id_type=MESH
        )
        return 0

    lax.fori_loop(1, size, one, 0)


def remote(src, dst, send, recv, device):
    return pltpu.make_async_remote_copy(
        src_ref=src, dst_ref=dst, send_sem=send, recv_sem=recv, device_id=device, device_id_type=MESH
    )


def fall_of(y):
    series = 1.0 + y * (1 / 6)
    for n in (5, 4, 3, 2):
        series = 1.0 + y * (1 / n) * series
    return jnp.where(y > -0.35, -y * series, 1.0 - jnp.exp(y))


def front_kernel(
    tp,
    sp,
    heads,
    begin,
    tok_ref,
    ngain_ref,
    wq,
    wk,
    wv,
    wri,
    wag,
    wrg,
    taps_ref,
    gr_ref,
    gi_ref,
    rate_ref,
    q_out,
    kv_out,
    ag_out,
    rg_out,
    prod_out,
    state_out,
    ends_out,
    w_buf,
    x_all,
    q_pack,
    kv_pack,
    ri_buf,
    tail_buf,
    early_buf,
    my_end,
    wsem,
    xs,
    xr,
    qs,
    qr,
    ks,
    kr,
    as_,
    ar,
    bs,
    br,
    hs,
    hr,
    es,
    er,
):
    me, col = lax.axis_index("sp"), lax.axis_index("tp")
    plane = sp // heads
    lanes = plane // 2
    z, r = lax.div(me, plane), lax.rem(me, plane)
    part_rows = tok_ref.shape[0]
    rows, width = prod_out.shape
    qw = q_out.shape[3]
    kvw = kv_out.shape[4]
    weights = [pltpu.make_async_copy(w, w_buf.at[n], wsem.at[n]) for n, w in enumerate((wq, wk, wv, wri, wag, wrg))]
    for copy in weights:
        copy.start()
    begin(True)
    greet("sp", sp)
    greet("tp", tp)
    x_all[col] = rms_rows(tok_ref[...].astype(jnp.float32), ngain_ref[...], EPS_INPUT).astype(jnp.bfloat16)
    pl.semaphore_wait(pltpu.get_barrier_semaphore(), sp + tp - 2)

    def give(k):
        return remote(x_all.at[col], x_all.at[col], xs.at[k], xr.at[k], {"tp": lax.rem(col + k, tp)})

    for k in range(1, tp):
        give(k).start()

    def dot(t, n):
        return jnp.dot(x_all[t], w_buf[n], preferred_element_type=jnp.float32).astype(jnp.bfloat16)

    def spread(k, s, t):
        there = {"sp": lax.rem(z + k, heads) * plane + r}
        n = k * tp + s
        g = lax.rem(z + k, heads)
        return (
            remote(kv_pack.at[g, s], kv_out.at[r, z, t], ks.at[n], kr.at[n], there),
            remote(q_pack.at[g, s], q_out.at[z, t], qs.at[n], qr.at[n], there),
        )

    def across(m, k, s, t):
        src = kv_out.at[r, lax.rem(z - k + heads, heads), t]
        n = (m * heads + k) * tp + s
        return remote(src, src, as_.at[n], ar.at[n], {"sp": z * plane + lax.rem(r + 2 * m, plane)})

    def twin(m, k, s, t):
        src = kv_out.at[lax.rem(r - 2 * m + plane, plane), lax.rem(z - k + heads, heads), t]
        n = (m * heads + k) * tp + s
        return remote(src, src, bs.at[n], br.at[n], {"sp": z * plane + r + 1 - 2 * lax.rem(r, 2)})

    def loop(low, high, fn):
        def one(m, _):
            fn(m)
            return 0

        lax.fori_loop(low, high, one, 0)

    def service(s, t):
        for k in range(heads):
            if k:
                spread(k, s, t)[0].wait_recv()
            loop(1, lanes, lambda m: across(m, k, s, t).start())
            twin(0, k, s, t).start()

    turns = [lax.rem(col - s + tp, tp) for s in range(tp)]
    for s, t in enumerate(turns):
        if s:
            give(s).wait_recv()
        if s == tp - 1:
            begin(False)
        at = pl.ds(pl.multiple_of(t * part_rows, part_rows), part_rows)
        for n in range(3):
            if s == 0:
                weights[n].wait()
            piece = dot(t, n)
            for g in range(heads):
                block = piece[:, g * qw : (g + 1) * qw]
                if n == 0:
                    q_pack[g, s] = block
                else:
                    kv_pack[g, s, :, (n - 1) * qw : n * qw] = block
        kv_out[r, z, t] = kv_pack[z, s]
        q_out[z, t] = q_pack[z, s]
        for k in range(1, heads):
            for copy in spread(k, s, t):
                copy.start()
        if s == 0:
            weights[3].wait()
        ri_buf[at] = dot(t, 3)
        if s:
            service(s - 1, turns[s - 1])
    tail_buf[...] = ri_buf[rows - 16 :]
    halo = remote(tail_buf, early_buf, hs, hr, {"sp": lax.rem(me + 1, sp)})
    halo.start()
    weights[4].wait()
    weights[5].wait()
    for t in range(tp):
        ag_out[t * part_rows : (t + 1) * part_rows] = dot(t, 4)
        rg_out[t * part_rows : (t + 1) * part_rows] = dot(t, 5)
    halo.wait()

    at = lax.broadcasted_iota(jnp.int32, (rows, width), 0)
    taps = taps_ref.shape[0]
    x = ri_buf[...].astype(jnp.float32)
    early = jnp.where(me == 0, 0.0, early_buf[...].astype(jnp.float32))
    conv = x * taps_ref[taps - 1][None]
    for back in range(1, taps):
        moved = pltpu.roll(x, back, 0)
        for row in range(back):
            moved = jnp.where(at == row, early[16 - back + row][None], moved)
        conv = conv + moved * taps_ref[taps - 1 - back][None]
    conv16 = conv.astype(jnp.bfloat16)
    size = gr_ref.shape[1]
    gates, flows = [], []
    for n in range(gr_ref.shape[0]):
        piece = conv16[:, n * size : (n + 1) * size]
        gates.append(jnp.dot(piece, gr_ref[n], preferred_element_type=jnp.float32))
        flows.append(jnp.dot(piece, gi_ref[n], preferred_element_type=jnp.float32))
    recur = jax.nn.sigmoid(jnp.concatenate(gates, axis=1))
    inflow = jax.nn.sigmoid(jnp.concatenate(flows, axis=1))
    log_decay = -RATE_SCALE * recur * rate_ref[...]
    a = jnp.exp(log_decay)
    norm_in = jnp.where((at == 0) & (me == 0), 1.0, jnp.sqrt(fall_of(2.0 * log_decay)))
    b = norm_in * inflow * conv16.astype(jnp.float32)
    shift = 1
    while shift < rows:
        keep = at >= shift
        pa = jnp.where(keep, pltpu.roll(a, shift, 0), 1.0)
        pb = jnp.where(keep, pltpu.roll(b, shift, 0), 0.0)
        b = b + a * pb
        a = a * pa
        shift *= 2
    prod_out[...] = a
    state_out[...] = b
    my_end[...] = jnp.zeros(my_end.shape, jnp.float32)
    my_end[0:1] = a[rows - 1 :]
    my_end[1:2] = b[rows - 1 :]
    ends_out[me] = my_end[...]

    def end(k):
        return remote(my_end, ends_out.at[me], es.at[k], er.at[k], {"sp": lax.rem(me + k, sp)})

    loop(1, sp, lambda k: end(k).start())
    service(tp - 1, turns[tp - 1])
    for s, t in enumerate(turns):
        for k in range(heads):

            def on(m):
                across(m, k, s, t).wait_recv()
                twin(m, k, s, t).start()

            loop(1, lanes, on)
    for s, t in enumerate(turns):
        for k in range(heads):
            if k:
                kv_copy, q_copy = spread(k, s, t)
                kv_copy.wait_send()
                q_copy.wait()
            loop(1, lanes, lambda m: across(m, k, s, t).wait_send())
            loop(0, lanes, lambda m: twin(m, k, s, t).wait())
    for k in range(1, tp):
        give(k).wait_send()
    loop(1, sp, lambda k: end(k).wait())


def layer_kernel(tp, sp, heads, *refs):
    lam_ref, gain_ref, oa_hbm, or_hbm, out_ref = refs[12:17]
    held, front_scratch = refs[17:24], refs[24:47]
    (
        oa,
        orr,
        m_ref,
        l_ref,
        acc_ref,
        o_stage,
        o_all,
        rec_part,
        p_stage,
        p_all,
        a_stage,
        a_all,
        wsem,
        osd,
        ord_,
        ps,
        pr,
        as_,
        ar,
        ws,
        wr,
        vs,
        vr,
    ) = refs[47:]
    q_ref, kv_ref, ag_ref, rg_ref, prod_ref, state_ref, ends_ref = held
    me, col = lax.axis_index("sp"), lax.axis_index("tp")
    plane = sp // heads
    z, r = lax.div(me, plane), lax.rem(me, plane)
    part_rows = q_ref.shape[2]
    rows = tp * part_rows
    width = q_ref.shape[3]
    half = width // 2
    cut = oa.shape[1] // 2
    side = pl.ds(pl.multiple_of(lax.rem(me, 2) * cut, cut), cut)
    w1 = pltpu.make_async_copy(oa_hbm, oa.at[col], wsem.at[0])
    w2 = pltpu.make_async_copy(or_hbm, orr, wsem.at[1])

    def share(k):
        block = oa.at[col, side]
        return remote(block, block, ws.at[k], wr.at[k], {"tp": lax.rem(col + k, tp)})

    def swap(k):
        block = oa.at[lax.rem(col - k + tp, tp), side]
        return remote(block, block, vs.at[k], vr.at[k], {"sp": me + 1 - 2 * lax.rem(me, 2)})

    def begin(early):
        if early:
            w1.start()
            w2.start()
            return
        w1.wait()
        for k in range(1, tp):
            share(k).start()

    front_kernel(tp, sp, heads, begin, *refs[:12], *held, *front_scratch)
    for k in range(1, tp):
        share(k).wait_recv()
        swap(k).start()
    lane = lax.broadcasted_iota(jnp.int32, (rows, width), 1)
    group = math.gcd(plane, 4)

    def give(k):
        g = lax.rem(z + k, heads)
        return remote(o_stage.at[g], o_all.at[z], osd.at[k], ord_.at[k], {"sp": g * plane + r})

    def attend(g):
        mine = g * plane + r
        q = q_ref[g].reshape(rows, width).astype(jnp.float32) * (half ** (-0.5))
        both = (
            jnp.where(lane < half, q, 0.0).astype(jnp.bfloat16),
            jnp.where(lane >= half, q, 0.0).astype(jnp.bfloat16),
        )
        m_ref[...] = jnp.full(m_ref.shape, MASKED, jnp.float32)
        l_ref[...] = jnp.zeros(l_ref.shape, jnp.float32)
        acc_ref[...] = jnp.zeros(acc_ref.shape, jnp.float32)

        def step(turn, masked):
            first = group * turn
            at, zz = lax.rem(first, plane), lax.div(first, plane)
            block = kv_ref[pl.ds(at, group), zz].reshape(group * rows, -1)
            keys, vals = block[:, :width], block[:, width:]
            scores = [
                lax.dot_general(
                    q_p, keys, (((1,), (1,)), ((), ())), preferred_element_type=jnp.float32
                )
                for q_p in both
            ]
            for p, s in enumerate(scores):
                if masked:
                    qpos = lax.broadcasted_iota(jnp.int32, s.shape, 0) + mine * rows
                    kpos = lax.broadcasted_iota(jnp.int32, s.shape, 1) + first * rows
                    s = jnp.where(kpos <= qpos, s, MASKED)
                old = m_ref[p]
                new = jnp.maximum(old, jnp.max(s, axis=-1, keepdims=True))
                factor = jnp.exp(old - new)
                e = jnp.exp(s - new[:, :1])
                m_ref[p] = new
                part = e[:, :128]
                for c in range(1, s.shape[1] // 128):
                    part = part + e[:, c * 128 : (c + 1) * 128]
                l_ref[p] = l_ref[p] * factor + part
                acc_ref[p] = acc_ref[p] * factor + jnp.dot(
                    e.astype(jnp.bfloat16), vals, preferred_element_type=jnp.float32
                )

        def body(turn, _):
            step(turn, False)
            return 0

        last = lax.div(mine, group)
        lax.fori_loop(0, last, body, 0)
        step(last, True)
        maps = [acc_ref[p] / jnp.sum(l_ref[p], axis=-1, keepdims=True) for p in range(2)]
        per_head = maps[0] - lam_ref[z] * maps[1]
        normal = rms_rows(per_head, gain_ref[pl.ds(z, 1)], EPS_HEAD) * HEAD_FACTOR
        return normal.astype(jnp.bfloat16)

    def hop(position, carry):
        longer = ends_ref[position, 0:1] * carry + ends_ref[position, 1:2]
        return jnp.where(position < me, longer, carry)

    carry = lax.fori_loop(0, sp - 1, hop, jnp.zeros((1, prod_ref.shape[1]), jnp.float32))
    states = state_ref[...] + prod_ref[...] * carry
    rec = (states * jax.nn.silu(rg_ref[...].astype(jnp.float32))).astype(jnp.bfloat16)
    w2.wait()
    rec_part[...] = jnp.dot(rec, orr[...], preferred_element_type=jnp.float32)

    def part_of(t):
        return pl.ds(pl.multiple_of(t * part_rows, part_rows), part_rows)

    def pass_on(k):
        t = lax.rem(col + k, tp)
        return remote(p_stage.at[t], p_all.at[col], ps.at[k], pr.at[k], {"tp": t})

    def mixed_on(k):
        t = lax.rem(col + k, tp)
        return remote(a_stage.at[t], a_all.at[col], as_.at[k], ar.at[k], {"tp": t})

    def mixed(t):
        at = part_of(t)
        att = jnp.concatenate([o_all[h, at] for h in range(heads)], axis=1).astype(jnp.float32)
        return (att * jax.nn.silu(ag_ref[at].astype(jnp.float32))).astype(jnp.bfloat16)

    for k in range(1, tp):
        t = lax.rem(col + k, tp)
        p_stage[t] = rec_part[part_of(t)].astype(jnp.bfloat16)
        pass_on(k).start()
    for k in list(range(1, heads)) + [0]:
        g = lax.rem(z + k, heads)
        done = attend(g)
        if k:
            o_stage[g] = done
            give(k).start()
        else:
            o_all[z] = done
    for k in range(1, heads):
        give(k).wait()
    for k in range(1, tp):
        t = lax.rem(col + k, tp)
        a_stage[t] = mixed(t)
        mixed_on(k).start()
    total = rec_part[part_of(col)] + jnp.dot(
        mixed(col), oa[col], preferred_element_type=jnp.float32
    )
    for k in range(1, tp):
        share(k).wait_send()
        swap(k).wait()
        pass_on(k).wait()
        total = total + p_all[lax.rem(col - k + tp, tp)].astype(jnp.float32)
    for k in range(1, tp):
        c = lax.rem(col - k + tp, tp)
        mixed_on(k).wait()
        total = total + jnp.dot(a_all[c], oa[c], preferred_element_type=jnp.float32)
    out_ref[...] = total.astype(jnp.bfloat16)


def body(
    tokens,
    norm_gain,
    w_query,
    w_key,
    w_value,
    w_att_gate,
    w_rec_in,
    w_rec_gate,
    conv_taps,
    gate_recur,
    gate_input,
    decay_rate,
    head_lambda,
    head_gain,
    out_att,
    out_rec,
):
    tp, sp, heads = lax.axis_size("tp"), lax.axis_size("sp"), head_lambda.shape[0]
    plane = sp // heads
    lanes = plane // 2
    part, depth = tokens.shape
    rows, width = part * tp, w_query.shape[1]
    qw, vdim = width // heads, w_value.shape[1] // heads
    kvw = qw + vdim
    chans = w_rec_in.shape[1]
    f32, b16 = jnp.float32, jnp.bfloat16
    shape = jax.ShapeDtypeStruct
    dma = pltpu.SemaphoreType.DMA
    steps = heads * tp
    return pl.pallas_call(
        functools.partial(layer_kernel, tp, sp, heads),
        out_shape=shape((part, out_att.shape[1]), b16),
        in_specs=[VMEM] * 2 + [ANY] * 6 + [VMEM] * 4 + [SMEM, VMEM, ANY, ANY],
        out_specs=VMEM,
        scratch_shapes=[
            pltpu.VMEM((heads, tp, part, qw), b16),
            pltpu.VMEM((plane, heads, tp, part, kvw), b16),
            pltpu.VMEM((rows, width), b16),
            pltpu.VMEM((rows, chans), b16),
            pltpu.VMEM((rows, chans), f32),
            pltpu.VMEM((rows, chans), f32),
            pltpu.VMEM((sp, 8, chans), f32),
            pltpu.VMEM((6, depth, width), b16),
            pltpu.VMEM((tp, part, depth), b16),
            pltpu.VMEM((heads, tp, part, qw), b16),
            pltpu.VMEM((heads, tp, part, kvw), b16),
            pltpu.VMEM((rows, chans), b16),
            pltpu.VMEM((16, chans), b16),
            pltpu.VMEM((16, chans), b16),
            pltpu.VMEM((8, chans), f32),
            dma((6,)),
            dma((tp,)),
            dma((tp,)),
            dma((steps,)),
            dma((steps,)),
            dma((steps,)),
            dma((steps,)),
            dma((lanes * steps,)),
            dma((lanes * steps,)),
            dma((lanes * steps,)),
            dma((lanes * steps,)),
            dma,
            dma,
            dma((sp,)),
            dma((sp,)),
            pltpu.VMEM((tp, *out_att.shape), b16),
            pltpu.VMEM(out_rec.shape, b16),
            pltpu.VMEM((2, rows, 128), f32),
            pltpu.VMEM((2, rows, 128), f32),
            pltpu.VMEM((2, rows, vdim), f32),
            pltpu.VMEM((heads, rows, vdim), b16),
            pltpu.VMEM((heads, rows, vdim), b16),
            pltpu.VMEM((rows, out_att.shape[1]), f32),
            pltpu.VMEM((tp, part, out_att.shape[1]), b16),
            pltpu.VMEM((tp, part, out_att.shape[1]), b16),
            pltpu.VMEM((tp, part, width), b16),
            pltpu.VMEM((tp, part, width), b16),
            dma((2,)),
            dma((heads,)),
            dma((heads,)),
            dma((tp,)),
            dma((tp,)),
            dma((tp,)),
            dma((tp,)),
            dma((tp,)),
            dma((tp,)),
            dma((tp,)),
            dma((tp,)),
        ],
        compiler_params=pltpu.CompilerParams(
            collective_id=0, has_side_effects=True, vmem_limit_bytes=LIMIT
        ),
        name="layer",
    )(
        tokens,
        norm_gain.reshape(1, depth),
        w_query,
        w_key,
        w_value,
        w_rec_in,
        w_att_gate,
        w_rec_gate,
        conv_taps,
        gate_recur,
        gate_input,
        decay_rate.reshape(1, chans),
        head_lambda,
        head_gain.reshape(heads, vdim),
        out_att,
        out_rec,
    )


def solution(mesh):
    return jax.shard_map(
        body,
        mesh=mesh,
        in_specs=(
            P(("sp", "tp"), None),
            P(),
            P(None, "tp"),
            P(None, "tp"),
            P(None, "tp"),
            P(None, "tp"),
            P(None, "tp"),
            P(None, "tp"),
            P(None, "tp"),
            P("tp", None, None),
            P("tp", None, None),
            P("tp"),
            P("tp"),
            P("tp"),
            P("tp", None),
            P("tp", None),
        ),
        out_specs=P(("sp", "tp"), None),
        check_vma=False,
    )
```

```python
import functools
import math

import jax
import jax.numpy as jnp
from jax import lax
from jax.experimental import pallas as pl
from jax.experimental.pallas import tpu as pltpu
from jax.sharding import PartitionSpec as P

EPS_INPUT = 1e-06
EPS_HEAD = 1e-05
RATE_SCALE = 8.0
HEAD_FACTOR = 0.8
MASKED = -1e30
MESH = pl.DeviceIdType.MESH
VMEM = pl.BlockSpec(memory_space=pltpu.VMEM)
ANY = pl.BlockSpec(memory_space=pl.ANY)
SMEM = pl.BlockSpec(memory_space=pltpu.SMEM)
LIMIT = 60 * 1024 * 1024


def rms_rows(values, gain, epsilon):
    mean_square = jnp.mean(values * values, axis=-1, keepdims=True)
    return values * lax.rsqrt(mean_square + epsilon) * gain


def greet(axis, size):
    barrier = pltpu.get_barrier_semaphore()
    me = lax.axis_index(axis)

    def one(k, _):
        pl.semaphore_signal(
            barrier, inc=1, device_id={axis: lax.rem(me + k, size)}, device_id_type=MESH
        )
        return 0

    lax.fori_loop(1, size, one, 0)


def remote(src, dst, send, recv, device):
    return pltpu.make_async_remote_copy(
        src_ref=src, dst_ref=dst, send_sem=send, recv_sem=recv, device_id=device, device_id_type=MESH
    )


def fall_of(y):
    series = 1.0 + y * (1 / 6)
    for n in (5, 4, 3, 2):
        series = 1.0 + y * (1 / n) * series
    return jnp.where(y > -0.35, -y * series, 1.0 - jnp.exp(y))


def front_kernel(
    tp,
    sp,
    heads,
    begin,
    tok_ref,
    ngain_ref,
    wq,
    wk,
    wv,
    wri,
    wag,
    wrg,
    taps_ref,
    gr_ref,
    gi_ref,
    rate_ref,
    q_out,
    kv_out,
    ag_out,
    rg_out,
    prod_out,
    state_out,
    ends_out,
    w_buf,
    x_all,
    q_pack,
    kv_pack,
    ri_buf,
    tail_buf,
    early_buf,
    my_end,
    wsem,
    xs,
    xr,
    qs,
    qr,
    ks,
    kr,
    as_,
    ar,
    bs,
    br,
    hs,
    hr,
    es,
    er,
):
    me, col = lax.axis_index("sp"), lax.axis_index("tp")
    plane = sp // heads
    lanes = plane // 2
    z, r = lax.div(me, plane), lax.rem(me, plane)
    part_rows = tok_ref.shape[0]
    rows, width = prod_out.shape
    qw = q_out.shape[3]
    kvw = kv_out.shape[4]
    weights = [pltpu.make_async_copy(w, w_buf.at[n], wsem.at[n]) for n, w in enumerate((wq, wk, wv, wri, wag, wrg))]
    for n in (1, 2, 0, 3, 4, 5):
        weights[n].start()
    begin(True)
    greet("sp", sp)
    greet("tp", tp)
    x_all[col] = rms_rows(tok_ref[...].astype(jnp.float32), ngain_ref[...], EPS_INPUT).astype(jnp.bfloat16)
    pl.semaphore_wait(pltpu.get_barrier_semaphore(), sp + tp - 2)

    def give(k):
        return remote(x_all.at[col], x_all.at[col], xs.at[k], xr.at[k], {"tp": lax.rem(col + k, tp)})

    for k in range(1, tp):
        give(k).start()

    def dot(t, n):
        return jnp.dot(x_all[t], w_buf[n], preferred_element_type=jnp.float32).astype(jnp.bfloat16)

    def spread(k, s, t):
        there = {"sp": lax.rem(z + k, heads) * plane + r}
        n = k * tp + s
        g = lax.rem(z + k, heads)
        return (
            remote(kv_pack.at[g, s], kv_out.at[r, z, t], ks.at[n], kr.at[n], there),
            remote(q_pack.at[g, s], q_out.at[z, t], qs.at[n], qr.at[n], there),
        )

    def across(m, k, s, t):
        src = kv_out.at[r, lax.rem(z - k + heads, heads), t]
        n = (m * heads + k) * tp + s
        return remote(src, src, as_.at[n], ar.at[n], {"sp": z * plane + lax.rem(r + 2 * m, plane)})

    def twin(m, k, s, t):
        src = kv_out.at[lax.rem(r - 2 * m + plane, plane), lax.rem(z - k + heads, heads), t]
        n = (m * heads + k) * tp + s
        return remote(src, src, bs.at[n], br.at[n], {"sp": z * plane + r + 1 - 2 * lax.rem(r, 2)})

    def loop(low, high, fn):
        def one(m, _):
            fn(m)
            return 0

        lax.fori_loop(low, high, one, 0)

    def service(s, t):
        for k in range(heads):
            if k:
                spread(k, s, t)[0].wait_recv()
            loop(1, lanes, lambda m: across(m, k, s, t).start())
            twin(0, k, s, t).start()

    turns = [lax.rem(col - s + tp, tp) for s in range(tp)]
    for s, t in enumerate(turns):
        if s:
            give(s).wait_recv()
        if s == tp - 1:
            begin(False)
        at = pl.ds(pl.multiple_of(t * part_rows, part_rows), part_rows)
        for n in (1, 2, 0):
            if s == 0:
                weights[n].wait()
            piece = dot(t, n)
            for g in range(heads):
                block = piece[:, g * qw : (g + 1) * qw]
                if n == 0:
                    q_pack[g, s] = block
                else:
                    kv_pack[g, s, :, (n - 1) * qw : n * qw] = block
            if n == 2:
                for k in range(1, heads):
                    spread(k, s, t)[0].start()
                kv_out[r, z, t] = kv_pack[z, s]
        for k in range(1, heads):
            spread(k, s, t)[1].start()
        q_out[z, t] = q_pack[z, s]
        if s == 0:
            weights[3].wait()
        ri_buf[at] = dot(t, 3)
        if s:
            service(s - 1, turns[s - 1])
    tail_buf[...] = ri_buf[rows - 16 :]
    halo = remote(tail_buf, early_buf, hs, hr, {"sp": lax.rem(me + 1, sp)})
    halo.start()
    weights[4].wait()
    weights[5].wait()
    for t in range(tp):
        ag_out[t * part_rows : (t + 1) * part_rows] = dot(t, 4)
        rg_out[t * part_rows : (t + 1) * part_rows] = dot(t, 5)
    halo.wait()

    at = lax.broadcasted_iota(jnp.int32, (rows, width), 0)
    taps = taps_ref.shape[0]
    x = ri_buf[...].astype(jnp.float32)
    early = jnp.where(me == 0, 0.0, early_buf[...].astype(jnp.float32))
    conv = x * taps_ref[taps - 1][None]
    for back in range(1, taps):
        moved = pltpu.roll(x, back, 0)
        for row in range(back):
            moved = jnp.where(at == row, early[16 - back + row][None], moved)
        conv = conv + moved * taps_ref[taps - 1 - back][None]
    conv16 = conv.astype(jnp.bfloat16)
    size = gr_ref.shape[1]
    gates, flows = [], []
    for n in range(gr_ref.shape[0]):
        piece = conv16[:, n * size : (n + 1) * size]
        gates.append(jnp.dot(piece, gr_ref[n], preferred_element_type=jnp.float32))
        flows.append(jnp.dot(piece, gi_ref[n], preferred_element_type=jnp.float32))
    recur = jax.nn.sigmoid(jnp.concatenate(gates, axis=1))
    inflow = jax.nn.sigmoid(jnp.concatenate(flows, axis=1))
    log_decay = -RATE_SCALE * recur * rate_ref[...]
    a = jnp.exp(log_decay)
    norm_in = jnp.where((at == 0) & (me == 0), 1.0, jnp.sqrt(fall_of(2.0 * log_decay)))
    b = norm_in * inflow * conv16.astype(jnp.float32)
    shift = 1
    while shift < rows:
        keep = at >= shift
        pa = jnp.where(keep, pltpu.roll(a, shift, 0), 1.0)
        pb = jnp.where(keep, pltpu.roll(b, shift, 0), 0.0)
        b = b + a * pb
        a = a * pa
        shift *= 2
    prod_out[...] = a
    state_out[...] = b
    my_end[...] = jnp.zeros(my_end.shape, jnp.float32)
    my_end[0:1] = a[rows - 1 :]
    my_end[1:2] = b[rows - 1 :]
    ends_out[me] = my_end[...]

    def end(k):
        return remote(my_end, ends_out.at[me], es.at[k], er.at[k], {"sp": lax.rem(me + k, sp)})

    loop(1, sp, lambda k: end(k).start())
    service(tp - 1, turns[tp - 1])
    for s, t in enumerate(turns):
        for k in range(heads):

            def on(m):
                across(m, k, s, t).wait_recv()
                twin(m, k, s, t).start()

            loop(1, lanes, on)
    for s, t in enumerate(turns):
        for k in range(heads):
            if k:
                kv_copy, q_copy = spread(k, s, t)
                kv_copy.wait_send()
                q_copy.wait()
            loop(1, lanes, lambda m: across(m, k, s, t).wait_send())
            loop(0, lanes, lambda m: twin(m, k, s, t).wait())
    for k in range(1, tp):
        give(k).wait_send()
    loop(1, sp, lambda k: end(k).wait())


def layer_kernel(tp, sp, heads, *refs):
    lam_ref, gain_ref, oa_hbm, or_hbm, out_ref = refs[12:17]
    held, front_scratch = refs[17:24], refs[24:47]
    (
        oa,
        orr,
        m_ref,
        l_ref,
        acc_ref,
        o_stage,
        o_all,
        rec_part,
        p_stage,
        p_all,
        a_stage,
        a_all,
        wsem,
        osd,
        ord_,
        ps,
        pr,
        as_,
        ar,
        ws,
        wr,
        vs,
        vr,
    ) = refs[47:]
    q_ref, kv_ref, ag_ref, rg_ref, prod_ref, state_ref, ends_ref = held
    me, col = lax.axis_index("sp"), lax.axis_index("tp")
    plane = sp // heads
    z, r = lax.div(me, plane), lax.rem(me, plane)
    part_rows = q_ref.shape[2]
    rows = tp * part_rows
    width = q_ref.shape[3]
    half = width // 2
    cut = oa.shape[1] // 2
    side = pl.ds(pl.multiple_of(lax.rem(me, 2) * cut, cut), cut)
    w1 = pltpu.make_async_copy(oa_hbm, oa.at[col], wsem.at[0])
    w2 = pltpu.make_async_copy(or_hbm, orr, wsem.at[1])

    def share(k):
        block = oa.at[col, side]
        return remote(block, block, ws.at[k], wr.at[k], {"tp": lax.rem(col + k, tp)})

    def swap(k):
        block = oa.at[lax.rem(col - k + tp, tp), side]
        return remote(block, block, vs.at[k], vr.at[k], {"sp": me + 1 - 2 * lax.rem(me, 2)})

    def begin(early):
        if early:
            w1.start()
            w2.start()
            return
        w1.wait()
        for k in range(1, tp):
            share(k).start()

    front_kernel(tp, sp, heads, begin, *refs[:12], *held, *front_scratch)
    for k in range(1, tp):
        share(k).wait_recv()
        swap(k).start()
    lane = lax.broadcasted_iota(jnp.int32, (rows, width), 1)
    group = math.gcd(plane, 4)

    def give(k):
        g = lax.rem(z + k, heads)
        return remote(o_stage.at[g], o_all.at[z], osd.at[k], ord_.at[k], {"sp": g * plane + r})

    def attend(g):
        mine = g * plane + r
        q = q_ref[g].reshape(rows, width).astype(jnp.float32) * (half ** (-0.5))
        both = (
            jnp.where(lane < half, q, 0.0).astype(jnp.bfloat16),
            jnp.where(lane >= half, q, 0.0).astype(jnp.bfloat16),
        )
        m_ref[...] = jnp.full(m_ref.shape, MASKED, jnp.float32)
        l_ref[...] = jnp.zeros(l_ref.shape, jnp.float32)
        acc_ref[...] = jnp.zeros(acc_ref.shape, jnp.float32)

        def step(turn, masked):
            first = group * turn
            at, zz = lax.rem(first, plane), lax.div(first, plane)
            block = kv_ref[pl.ds(at, group), zz].reshape(group * rows, -1)
            keys, vals = block[:, :width], block[:, width:]
            scores = [
                lax.dot_general(
                    q_p, keys, (((1,), (1,)), ((), ())), preferred_element_type=jnp.float32
                )
                for q_p in both
            ]
            for p, s in enumerate(scores):
                if masked:
                    qpos = lax.broadcasted_iota(jnp.int32, s.shape, 0) + mine * rows
                    kpos = lax.broadcasted_iota(jnp.int32, s.shape, 1) + first * rows
                    s = jnp.where(kpos <= qpos, s, MASKED)
                old = m_ref[p]
                new = jnp.maximum(old, jnp.max(s, axis=-1, keepdims=True))
                factor = jnp.exp(old - new)
                e = jnp.exp(s - new[:, :1])
                m_ref[p] = new
                part = e[:, :128]
                for c in range(1, s.shape[1] // 128):
                    part = part + e[:, c * 128 : (c + 1) * 128]
                l_ref[p] = l_ref[p] * factor + part
                acc_ref[p] = acc_ref[p] * factor + jnp.dot(
                    e.astype(jnp.bfloat16), vals, preferred_element_type=jnp.float32
                )

        def body(turn, _):
            step(turn, False)
            return 0

        last = lax.div(mine, group)
        lax.fori_loop(0, last, body, 0)
        step(last, True)
        maps = [acc_ref[p] / jnp.sum(l_ref[p], axis=-1, keepdims=True) for p in range(2)]
        per_head = maps[0] - lam_ref[z] * maps[1]
        normal = rms_rows(per_head, gain_ref[pl.ds(z, 1)], EPS_HEAD) * HEAD_FACTOR
        return normal.astype(jnp.bfloat16)

    def hop(position, carry):
        longer = ends_ref[position, 0:1] * carry + ends_ref[position, 1:2]
        return jnp.where(position < me, longer, carry)

    carry = lax.fori_loop(0, sp - 1, hop, jnp.zeros((1, prod_ref.shape[1]), jnp.float32))
    states = state_ref[...] + prod_ref[...] * carry
    rec = (states * jax.nn.silu(rg_ref[...].astype(jnp.float32))).astype(jnp.bfloat16)
    w2.wait()
    rec_part[...] = jnp.dot(rec, orr[...], preferred_element_type=jnp.float32)

    def part_of(t):
        return pl.ds(pl.multiple_of(t * part_rows, part_rows), part_rows)

    def pass_on(k):
        t = lax.rem(col + k, tp)
        return remote(p_stage.at[t], p_all.at[col], ps.at[k], pr.at[k], {"tp": t})

    def mixed_on(k):
        t = lax.rem(col + k, tp)
        return remote(a_stage.at[t], a_all.at[col], as_.at[k], ar.at[k], {"tp": t})

    def mixed(t):
        at = part_of(t)
        att = jnp.concatenate([o_all[h, at] for h in range(heads)], axis=1).astype(jnp.float32)
        return (att * jax.nn.silu(ag_ref[at].astype(jnp.float32))).astype(jnp.bfloat16)

    for k in range(1, tp):
        t = lax.rem(col + k, tp)
        p_stage[t] = rec_part[part_of(t)].astype(jnp.bfloat16)
        pass_on(k).start()
    for k in list(range(1, heads)) + [0]:
        g = lax.rem(z + k, heads)
        done = attend(g)
        if k:
            o_stage[g] = done
            give(k).start()
        else:
            o_all[z] = done
    for k in range(1, heads):
        give(k).wait()
    for k in range(1, tp):
        t = lax.rem(col + k, tp)
        a_stage[t] = mixed(t)
        mixed_on(k).start()
    total = rec_part[part_of(col)] + jnp.dot(
        mixed(col), oa[col], preferred_element_type=jnp.float32
    )
    for k in range(1, tp):
        share(k).wait_send()
        swap(k).wait()
        pass_on(k).wait()
        total = total + p_all[lax.rem(col - k + tp, tp)].astype(jnp.float32)
    for k in range(1, tp):
        c = lax.rem(col - k + tp, tp)
        mixed_on(k).wait()
        total = total + jnp.dot(a_all[c], oa[c], preferred_element_type=jnp.float32)
    out_ref[...] = total.astype(jnp.bfloat16)


def body(
    tokens,
    norm_gain,
    w_query,
    w_key,
    w_value,
    w_att_gate,
    w_rec_in,
    w_rec_gate,
    conv_taps,
    gate_recur,
    gate_input,
    decay_rate,
    head_lambda,
    head_gain,
    out_att,
    out_rec,
):
    tp, sp, heads = lax.axis_size("tp"), lax.axis_size("sp"), head_lambda.shape[0]
    plane = sp // heads
    lanes = plane // 2
    part, depth = tokens.shape
    rows, width = part * tp, w_query.shape[1]
    qw, vdim = width // heads, w_value.shape[1] // heads
    kvw = qw + vdim
    chans = w_rec_in.shape[1]
    f32, b16 = jnp.float32, jnp.bfloat16
    shape = jax.ShapeDtypeStruct
    dma = pltpu.SemaphoreType.DMA
    steps = heads * tp
    return pl.pallas_call(
        functools.partial(layer_kernel, tp, sp, heads),
        out_shape=shape((part, out_att.shape[1]), b16),
        in_specs=[VMEM] * 2 + [ANY] * 6 + [VMEM] * 4 + [SMEM, VMEM, ANY, ANY],
        out_specs=VMEM,
        scratch_shapes=[
            pltpu.VMEM((heads, tp, part, qw), b16),
            pltpu.VMEM((plane, heads, tp, part, kvw), b16),
            pltpu.VMEM((rows, width), b16),
            pltpu.VMEM((rows, chans), b16),
            pltpu.VMEM((rows, chans), f32),
            pltpu.VMEM((rows, chans), f32),
            pltpu.VMEM((sp, 8, chans), f32),
            pltpu.VMEM((6, depth, width), b16),
            pltpu.VMEM((tp, part, depth), b16),
            pltpu.VMEM((heads, tp, part, qw), b16),
            pltpu.VMEM((heads, tp, part, kvw), b16),
            pltpu.VMEM((rows, chans), b16),
            pltpu.VMEM((16, chans), b16),
            pltpu.VMEM((16, chans), b16),
            pltpu.VMEM((8, chans), f32),
            dma((6,)),
            dma((tp,)),
            dma((tp,)),
            dma((steps,)),
            dma((steps,)),
            dma((steps,)),
            dma((steps,)),
            dma((lanes * steps,)),
            dma((lanes * steps,)),
            dma((lanes * steps,)),
            dma((lanes * steps,)),
            dma,
            dma,
            dma((sp,)),
            dma((sp,)),
            pltpu.VMEM((tp, *out_att.shape), b16),
            pltpu.VMEM(out_rec.shape, b16),
            pltpu.VMEM((2, rows, 128), f32),
            pltpu.VMEM((2, rows, 128), f32),
            pltpu.VMEM((2, rows, vdim), f32),
            pltpu.VMEM((heads, rows, vdim), b16),
            pltpu.VMEM((heads, rows, vdim), b16),
            pltpu.VMEM((rows, out_att.shape[1]), f32),
            pltpu.VMEM((tp, part, out_att.shape[1]), b16),
            pltpu.VMEM((tp, part, out_att.shape[1]), b16),
            pltpu.VMEM((tp, part, width), b16),
            pltpu.VMEM((tp, part, width), b16),
            dma((2,)),
            dma((heads,)),
            dma((heads,)),
            dma((tp,)),
            dma((tp,)),
            dma((tp,)),
            dma((tp,)),
            dma((tp,)),
            dma((tp,)),
            dma((tp,)),
            dma((tp,)),
        ],
        compiler_params=pltpu.CompilerParams(
            collective_id=0, has_side_effects=True, vmem_limit_bytes=LIMIT
        ),
        name="layer",
    )(
        tokens,
        norm_gain.reshape(1, depth),
        w_query,
        w_key,
        w_value,
        w_rec_in,
        w_att_gate,
        w_rec_gate,
        conv_taps,
        gate_recur,
        gate_input,
        decay_rate.reshape(1, chans),
        head_lambda,
        head_gain.reshape(heads, vdim),
        out_att,
        out_rec,
    )


def solution(mesh):
    return jax.shard_map(
        body,
        mesh=mesh,
        in_specs=(
            P(("sp", "tp"), None),
            P(),
            P(None, "tp"),
            P(None, "tp"),
            P(None, "tp"),
            P(None, "tp"),
            P(None, "tp"),
            P(None, "tp"),
            P(None, "tp"),
            P("tp", None, None),
            P("tp", None, None),
            P("tp"),
            P("tp"),
            P("tp"),
            P("tp", None),
            P("tp", None),
        ),
        out_specs=P(("sp", "tp"), None),
        check_vma=False,
    )
```
